512 devices in a mesh: sp: 16 (over y, x), tp: 32 (over z, core).
Axes of the slice: x: 4, y: 4, z: 16, core: 2. Of those that a mesh axis runs over, the one named last changes fastest.
Arguments:
- tokens: bfloat16 [32, 2048, 4096], P('tp', 'sp'), may hold values from -6 to 6
- latent_down_matrix: bfloat16 [4096, 512], P('tp'), may hold values from -0.09375 to 0.09375
- rope_weight: bfloat16 [4096, 64], P('tp'), may hold values from -0.09375 to 0.09375
- latent_norm_scale: float32 [512], replicated, may hold values from 0.1 to 1.9
- key_up_matrix: bfloat16 [512, 32, 128], P(None, 'tp'), may hold values from -0.25 to 0.25
- value_up_matrix: bfloat16 [512, 32, 128], P(None, 'tp'), may hold values from -0.25 to 0.25
- query: bfloat16 [32, 32, 192], P('sp', 'tp'), may hold values from -126 to 126
Outputs:
- plain_key_cache: bfloat16 [32, 2048, 32, 128], P('sp', None, 'tp')
- head_value_cache: bfloat16 [32, 2048, 32, 128], P('sp', None, 'tp')
- rotated_key_cache: bfloat16 [32, 2048, 64], P('sp')
- first_read: bfloat16 [32, 32, 128], P('sp', 'tp')
The draws below stay inside these ranges and needn't reach their ends.
All inputs are finite; a program needn't handle non-finite values.
Results may differ from the reference program's by a relative error of at most 0.035.
Values may be sent and summed in bfloat16 or wider, within the bound.
A program may use at most 64 MiB of HBM per device.

```python
import jax
import jax.numpy as jnp
from jax import lax

MODEL_WIDTH = 4096
LATENT_WIDTH = 512
ROPE = 64
PLAIN_KEY_WIDTH = 128
VALUE_WIDTH = 128
ATTENTION_HEADS = 32
SEQUENCE_COUNT = 32
SEQUENCE_LENGTH = 2048


def draw_query(key, part):
    base = jnp.clip(jax.random.normal(jax.random.fold_in(key, 11), (SEQUENCE_COUNT, ATTENTION_HEADS, PLAIN_KEY_WIDTH + ROPE), jnp.float32), -3.5, 3.5) * 3.0
    return base.astype(jnp.bfloat16)


def block_scale(key, dims, split, least, top_value):
    level = 1.0
    for dim, parts in split:
        heights = jax.random.uniform(jax.random.fold_in(jax.random.fold_in(key, 6), dim), (parts,), jnp.float32, least / len(split), top_value / len(split))
        level = level * jnp.repeat(jnp.exp(heights), dims[dim] // parts).reshape((-1,) + (1,) * (len(dims) - 1 - dim))
    return level


def gaussian(rng, shape, scale, most, cuts=(), kind=jnp.bfloat16):
    factor_of = block_scale(rng, shape, cuts, -0.22, 0.18) if cuts else 1.0
    array = jax.random.normal(rng, shape, jnp.float32) * scale * factor_of
    return jnp.minimum(jnp.maximum(array, -most), most).astype(kind)


def setup_inputs(seed: int = 0) -> dict:
    key_list = jax.random.split(jax.random.key(seed), 8)
    return {
        "tokens": gaussian(key_list[0], (SEQUENCE_COUNT, SEQUENCE_LENGTH, MODEL_WIDTH), 1.0, 6.0, ((0, 32), (1, 16))),
        "latent_down_matrix": gaussian(key_list[1], (MODEL_WIDTH, LATENT_WIDTH), MODEL_WIDTH ** -0.5, 0.09375, ((0, 32),)),
        "rope_weight": gaussian(key_list[2], (MODEL_WIDTH, ROPE), MODEL_WIDTH ** -0.5, 0.09375, ((0, 32),)),
        "latent_norm_scale": jnp.clip(1.0 + 0.18 * jax.random.normal(key_list[3], (LATENT_WIDTH,), jnp.float32), 0.1, 1.9),
        "key_up_matrix": gaussian(key_list[4], (LATENT_WIDTH, ATTENTION_HEADS, PLAIN_KEY_WIDTH), LATENT_WIDTH ** -0.5, 0.25, ((1, 32),)),
        "value_up_matrix": gaussian(key_list[5], (LATENT_WIDTH, ATTENTION_HEADS, VALUE_WIDTH), LATENT_WIDTH ** -0.5, 0.25, ((1, 32),)),
        "query": draw_query(jax.random.fold_in(key_list[7], 71), 0),
    }


def rotate(part, positions):
    half = part.shape[-1] // 2
    freqs = 1.0 / 10000.0 ** (jnp.arange(half, dtype=jnp.float32) * 2.0 / part.shape[-1])
    angles = positions.astype(jnp.float32)[:, None] * freqs
    cosine = jnp.cos(angles)
    sine = jnp.sin(angles)
    first = part[..., :half]
    second = part[..., half:]
    return jnp.concatenate([first * cosine - second * sine, second * cosine + first * sine], axis=-1)

def reference(tokens, latent_down_matrix, rope_weight, latent_norm_scale, key_up_matrix, value_up_matrix, query):
    flat = tokens.reshape(SEQUENCE_COUNT * SEQUENCE_LENGTH, MODEL_WIDTH)
    latent = jnp.dot(flat, latent_down_matrix, preferred_element_type=jnp.float32)
    scaled = latent * lax.rsqrt(lax.optimization_barrier(jnp.mean(latent * latent, axis=-1, keepdims=True)) + 1e-06)
    latent_normalized = (scaled * latent_norm_scale.astype(jnp.float32)).astype(jnp.bfloat16)
    rope = jnp.dot(flat, rope_weight, preferred_element_type=jnp.float32).reshape(SEQUENCE_COUNT, SEQUENCE_LENGTH, ROPE)
    positions = jnp.arange(SEQUENCE_LENGTH, dtype=jnp.int32)
    rotated_key_cache = rotate(rope, positions).astype(jnp.bfloat16)
    plain_key_cache = jnp.dot(latent_normalized, key_up_matrix.reshape(LATENT_WIDTH, ATTENTION_HEADS * PLAIN_KEY_WIDTH), preferred_element_type=jnp.float32).astype(jnp.bfloat16).reshape(SEQUENCE_COUNT, SEQUENCE_LENGTH, ATTENTION_HEADS, PLAIN_KEY_WIDTH)
    head_value_cache = jnp.dot(latent_normalized, value_up_matrix.reshape(LATENT_WIDTH, ATTENTION_HEADS * VALUE_WIDTH), preferred_element_type=jnp.float32).astype(jnp.bfloat16).reshape(SEQUENCE_COUNT, SEQUENCE_LENGTH, ATTENTION_HEADS, VALUE_WIDTH)
    query_float = query.astype(jnp.float32)
    query_plain = query[..., :PLAIN_KEY_WIDTH]
    rotated_query = rotate(query_float[..., PLAIN_KEY_WIDTH:], jnp.full((1,), SEQUENCE_LENGTH, jnp.int32)).astype(jnp.bfloat16)
    factor = 1.0 / (PLAIN_KEY_WIDTH + ROPE) ** 0.5

    def attend(items):
        plain, turned, keys, values, rotary = items
        scores = jnp.einsum('hd,lhd->hl', plain.astype(jnp.float32), keys.astype(jnp.float32))
        scores = scores + jnp.einsum('hd,ld->hl', turned.astype(jnp.float32), rotary.astype(jnp.float32))
        scores = scores * factor
        weights = jnp.exp(scores - lax.optimization_barrier(jnp.max(scores, axis=-1, keepdims=True)))
        total = lax.optimization_barrier(jnp.sum(weights, axis=-1, keepdims=True))
        rounded = weights.astype(jnp.bfloat16)
        mixed = jnp.einsum('hl,lhd->hd', rounded.astype(jnp.float32), values.astype(jnp.float32))
        return (mixed / total).astype(jnp.bfloat16)
    first_read = lax.map(attend, (query_plain, rotated_query, plain_key_cache, head_value_cache, rotated_key_cache))
    return (plain_key_cache, head_value_cache, rotated_key_cache, first_read)
```

```python
import functools

import numpy as np
import jax
import jax.numpy as jnp
from jax import lax
from jax.sharding import PartitionSpec as P
from jax.experimental import pallas as pl
from jax.experimental.pallas import tpu as pltpu

CORES = 2
SIDE = 4
PARTS = 4
BF16 = jnp.bfloat16
F32 = jnp.float32


def turn_tables(positions, width):
    half = width // 2
    freqs = (1.0 / np.float32(10000.0) ** (np.arange(half, dtype=np.float32) * np.float32(2.0) / np.float32(width))).astype(np.float32)
    angles = positions.astype(np.float32)[:, None] * freqs
    cosine = np.cos(angles).astype(np.float32)
    sine = np.sin(angles).astype(np.float32)
    return np.concatenate([cosine, cosine], -1), np.concatenate([-sine, sine], -1)


def turn(part, cosine, sine):
    half = part.shape[-1] // 2
    swapped = jnp.concatenate([part[:, half:], part[:, :half]], axis=-1)
    return part * cosine + swapped * sine


def move_kernel(planes, spots, tok, wl, wr, scale, cos_hbm, sin_hbm, fin, fint,
                tokens, wlat, wrope, acc, acct, other, othert, own, ownt, trans, transt, cos_ref, sin_ref,
                tok_s, tok_r, own_s, z_s, z_r, a_s, a_r, b_s, b_r, t_s, t_r,
                acc_s, acc_r, x_s, x_r, up_s, down_s, in_r, y_s, y_r, p_s, p_r):
    s = lax.axis_index("sp")
    t = lax.axis_index("tp")
    z = t // CORES
    c = t % CORES
    x = s % SIDE
    y = s // SIDE
    rows, lat = wl.shape
    rope = wr.shape[0]
    span = tok.shape[1]
    rcut = rows // SIDE
    lcut = lat // SIDE
    pcut = rope // SIDE
    cut = span // PARTS
    far = planes // 2

    def dev(yi, xi, zi, ci):
        return {"sp": yi * SIDE + xi, "tp": zi * CORES + ci}

    here = dev(y, x, z, 1 - c)

    def around(v, n):
        return lax.rem(v + n, n)

    def remote(src, dst, ss, rs, where):
        return pltpu.make_async_remote_copy(
            src_ref=src, dst_ref=dst, send_sem=ss, recv_sem=rs,
            device_id=where, device_id_type=pl.DeviceIdType.MESH)

    def each(copies, what):
        for p in copies:
            getattr(p, what)()

    def own_tok(u):
        cols = pl.ds(pl.multiple_of((u * CORES + c) * rows, 128), rows)
        return pltpu.make_async_copy(tok.at[0, :, cols], tokens.at[0, u], own_s.at[u])

    def part_tok(u):
        cols = pl.ds(pl.multiple_of((u * CORES + 1 - c) * rows, 128), rows)
        return remote(tok.at[0, :, cols], tokens.at[1, u], tok_s.at[u], tok_r.at[u], here)

    own_wl = pltpu.make_async_copy(wl, wlat.at[z], own_s.at[planes])
    own_wr = pltpu.make_async_copy(wr, wrope.at[z], own_s.at[planes + 1])
    place = pl.ds(pl.multiple_of(s * span, 128), span)
    get_c = pltpu.make_async_copy(cos_hbm.at[:, place], cos_ref, own_s.at[planes + 2])
    get_n = pltpu.make_async_copy(sin_hbm.at[:, place], sin_ref, own_s.at[planes + 3])
    own_wl.start()
    own_wr.start()

    barrier = pltpu.get_barrier_semaphore()

    def greet(where):
        pl.semaphore_signal(barrier, inc=1, device_id=where, device_id_type=pl.DeviceIdType.MESH)

    for i in range(1, planes):
        greet(dev(y, x, around(z + i, planes), c))
    for i in range(1, SIDE):
        greet(dev(y, around(x + i, SIDE), z, c))
        greet(dev(around(y + i, SIDE), x, z, c))
    greet(here)
    for u in range(planes):
        own_tok(u).start()
    get_c.start()
    get_n.start()
    own_wl.wait()
    own_wr.wait()
    pl.semaphore_wait(barrier, planes - 1 + 2 * (SIDE - 1) + 1)

    def w_piece(u):
        return wlat.at[u, pl.ds(pl.multiple_of(y * rcut, 16), rcut), pl.ds(pl.multiple_of(x * lcut, 128), lcut)]

    def w_row(u):
        return wlat.at[u, pl.ds(pl.multiple_of(y * rcut, 16), rcut)]

    def w_col(u):
        return wlat.at[u, :, pl.ds(pl.multiple_of(x * lcut, 128), lcut)]

    def r_piece(u, i):
        return wrope.at[u, pl.ds(pl.multiple_of(i * pcut, 16), pcut)]

    def z_copy(u, zi, i):
        where = dev(y, x, zi, c)
        return [remote(w_piece(u), w_piece(u), z_s.at[0, zi], z_r.at[0, u], where),
                remote(r_piece(u, i), r_piece(u, i), z_s.at[1, zi], z_r.at[1, u], where)]

    def a_copy(u, o, by_row):
        where = dev(y, around(x + o, SIDE), z, c) if by_row else dev(around(y + o, SIDE), x, z, c)
        return remote(w_piece(u), w_piece(u), a_s.at[o - 1, u], a_r.at[o - 1, u], where)

    def b_copy(u, o, by_row):
        where = dev(around(y + o, SIDE), x, z, c) if by_row else dev(y, around(x + o, SIDE), z, c)
        part = w_row(u) if by_row else w_col(u)
        turned = r_piece(u, y if by_row else x)
        return [remote(part, part, b_s.at[o - 1, u], b_r.at[o - 1, u], where),
                remote(turned, turned, t_s.at[o - 1, u], t_r.at[o - 1, u], where)]

    def below(d):
        return around(z - d, planes)

    def above(d):
        return around(z + d, planes)

    def z_send(d, carry):
        each(z_copy(z, above(d), y), "start")

        @pl.when(d < far)
        def _():
            each(z_copy(z, below(d), x), "start")
        return carry

    lax.fori_loop(1, far + 1, z_send, 0)
    for u in range(planes):
        part_tok(u).start()

    contract = (((1,), (1,)), ((), ()))

    def block_dot(u):
        v = tokens[:, u].reshape(CORES * span, rows)
        return (jnp.dot(v, wlat[u], preferred_element_type=F32),
                lax.dot_general(wrope[u], v, contract, preferred_element_type=F32))

    def own_block():
        for u in range(planes):
            own_tok(u).wait()
            part_tok(u).wait()
        a, b = block_dot(z)
        acc[...] = a
        acct[...] = b

    def first(u, by_row):
        z_copy(u, z, y)[0].wait_recv()
        for o in range(1, SIDE):
            a_copy(u, o, by_row).start()

    def second(u, by_row):
        z_copy(u, z, y)[1].wait_recv()
        for o in range(1, SIDE):
            a_copy(u, o, by_row).wait_recv()
        for o in range(1, SIDE):
            each(b_copy(u, o, by_row), "start")

    def third(u, by_row):
        for o in range(1, SIDE):
            each(b_copy(u, o, by_row), "wait_recv")
        a, b = block_dot(u)
        acc[...] += a
        acct[...] += b

    def both(d, what):
        @pl.when((d >= 1) & (d <= far))
        def _():
            what(below(d), True)

        @pl.when((d >= 1) & (d < far))
        def _():
            what(above(d), False)

    def step(i, carry):
        both(i, first)
        both(i - 2, second)

        @pl.when(i == 3)
        def _():
            own_block()

        both(i - 4, third)
        return carry

    lax.fori_loop(1, far + 5, step, 0)

    swaps = [remote(acc.at[pl.ds(span, span)], other, acc_s.at[0], acc_r.at[0], here),
             remote(acct.at[:, pl.ds(span, span)], othert, acc_s.at[1], acc_r.at[1], here)]
    each(swaps, "start")
    get_c.wait()
    get_n.wait()
    each(swaps, "wait")
    latent = acc[:span] + other[...]
    ropes = acct[:, :span] + othert[...]
    scaled = latent * lax.rsqrt(jnp.mean(latent * latent, axis=-1, keepdims=True) + 1e-06)
    normed = (scaled * scale[...]).astype(BF16)
    swapped = jnp.concatenate([ropes[rope // 2:], ropes[:rope // 2]], axis=0)
    rotated = (ropes * cos_ref[...] + swapped * sin_ref[...]).astype(BF16)

    xq = z % SIDE
    kq = z // SIDE
    origin = x == xq

    @pl.when(origin)
    def _():
        trans[kq * SIDE + x] = normed
        transt[kq * SIDE + x] = rotated

    @pl.when(~origin)
    def _():
        own[...] = normed
        ownt[...] = rotated

    def chunk(p):
        return pl.ds(p * cut, cut)

    def x_copy(xs, p):
        slot = kq * SIDE + xs
        where = dev(y, xq, z, c)
        out = [remote(own.at[chunk(p)], trans.at[slot, chunk(p)], x_s.at[p], x_r.at[p, xs], where)]
        if p == 0:
            out.append(remote(ownt, transt.at[slot], x_s.at[PARTS], x_r.at[PARTS, xs], where))
        return out

    def z_move(slot, p, zi, sems):
        where = dev(y, x, zi, c)
        out = [remote(trans.at[slot, chunk(p)], trans.at[slot, chunk(p)], sems.at[p, slot], in_r.at[p, slot], where)]
        if p == 0:
            out.append(remote(transt.at[slot], transt.at[slot], sems.at[PARTS, slot], in_r.at[PARTS, slot], where))
        return out

    def up_move(slot, p):
        return z_move(slot, p, around(z + 1, planes), up_s)

    def down_move(slot, p):
        return z_move(slot, p, around(z - 1, planes), down_s)

    def y_move(k, xs, p, place):
        slot = k * SIDE + xs
        where = dev(k, x, z, c)
        out = [remote(trans.at[slot, chunk(p)], fin.at[c, place, chunk(p)], y_s.at[p, slot], y_r.at[p, place], where)]
        if p == 0:
            out.append(remote(transt.at[slot], fint.at[c, place], y_s.at[PARTS, slot], y_r.at[PARTS, place], where))
        return out

    def p_from(src, srct, place, p):
        out = [remote(src, fin.at[c, place, chunk(p)], p_s.at[p, place], p_r.at[p, place], here)]
        if p == 0:
            out.append(remote(srct, fint.at[c, place], p_s.at[PARTS, place], p_r.at[PARTS, place], here))
        return out

    def p_pass(place, p):
        return p_from(fin.at[c, place, chunk(p)], fint.at[c, place], place, p)

    def p_keep(xs, p):
        slot = y * SIDE + xs
        return p_from(trans.at[slot, chunk(p)], transt.at[slot], slot, p)

    def p_in(place, p):
        mine = [remote(fin.at[1 - c, place, chunk(p)], fin.at[1 - c, place, chunk(p)], p_s.at[p, place], p_r.at[p, place], here)]
        if p == 0:
            mine.append(remote(fint.at[1 - c, place], fint.at[1 - c, place], p_s.at[PARTS, place], p_r.at[PARTS, place], here))
        return mine

    early = PARTS // 2

    def goes_up(f, p):
        return (f < far - 1) | (f == far - 1) if p < early else f < far - 1

    def goes_down(f, p):
        return f < far - 1 if p < early else (f < far - 1) | (f == far - 1)

    def hand_over(k, xs, p):
        @pl.when(k != y)
        def _():
            each(y_move(k, xs, p, y * SIDE + xs), "start")

        @pl.when(k == y)
        def _():
            slot = k * SIDE + xs
            each(p_keep(xs, p), "start")
            fin[c, slot, p * cut:(p + 1) * cut] = trans[slot, p * cut:(p + 1) * cut]
            if p == 0:
                fint[c, slot] = transt[slot]

    @pl.when(~origin)
    def _():
        for p in range(PARTS):
            each(x_copy(x, p), "start")

    e = lax.rem(z - x + planes, SIDE)
    lower = jnp.where(e == 0, SIDE, e)
    upper = SIDE - e

    def ring(i, carry):
        ib = i - lower
        ia = i - upper
        db = lower + SIDE * (ib // SIDE)
        da = upper + SIDE * (ia // SIDE)
        kb = around(z - db, planes) // SIDE
        ka = around(z + da, planes) // SIDE
        xb = lax.rem(ib + SIDE, SIDE)
        xa = lax.rem(ia + SIDE, SIDE)
        for p in range(PARTS):
            @pl.when(origin & (i < SIDE))
            def _():
                xs = lax.rem(x + i, SIDE)
                slot = kq * SIDE + xs

                @pl.when(i > 0)
                def _():
                    each(x_copy(xs, p), "wait_recv")
                each(up_move(slot, p), "start")
                each(down_move(slot, p), "start")
                hand_over(kq, xs, p)

            @pl.when((ib >= 0) & (ib < 2 * SIDE) & ((db < far) | (p < early)))
            def _():
                slot = kb * SIDE + lax.rem(x + xb, SIDE)
                each(up_move(slot, p), "wait_recv")

                @pl.when(goes_up(db, p))
                def _():
                    each(up_move(slot, p), "start")
                hand_over(kb, lax.rem(x + xb, SIDE), p)

            @pl.when((ia >= 0) & (ia < 2 * SIDE) & ((da < far) | (p >= early)))
            def _():
                slot = ka * SIDE + lax.rem(x + xa, SIDE)
                each(down_move(slot, p), "wait_recv")

                @pl.when(goes_down(da, p))
                def _():
                    each(down_move(slot, p), "start")
                hand_over(ka, lax.rem(x + xa, SIDE), p)
        return carry

    lax.fori_loop(0, 3 * SIDE, ring, 0)

    def pass_on(xs, carry):
        for p in range(PARTS):
            for o in range(1, SIDE):
                place = around(y + o, SIDE) * SIDE + xs
                each(y_move(y, xs, p, place), "wait_recv")
                each(p_pass(place, p), "start")
        return carry

    lax.fori_loop(0, SIDE, pass_on, 0)

    def drain(i, carry):
        k = i // SIDE
        xs = lax.rem(i, SIDE)
        u = x + k * SIDE
        f = around(z - u, planes)
        g = around(u - z, planes)
        for p in range(PARTS):
            each(p_in(i, p), "wait_recv")
            each(p_pass(i, p), "wait_send")

            @pl.when(goes_up(f, p))
            def _():
                each(up_move(i, p), "wait_send")

            @pl.when(goes_down(g, p))
            def _():
                each(down_move(i, p), "wait_send")

            @pl.when(k != y)
            def _():
                each(y_move(k, xs, p, y * SIDE + xs), "wait_send")
        return carry

    lax.fori_loop(0, spots, drain, 0)

    @pl.when(~origin)
    def _():
        for p in range(PARTS):
            each(x_copy(x, p), "wait_send")

    def settle(d, carry):
        each(z_copy(z, above(d), y), "wait_send")

        def sent(u, by_row):
            for o in range(1, SIDE):
                a_copy(u, o, by_row).wait_send()
                each(b_copy(u, o, by_row), "wait_send")

        sent(below(d), True)

        @pl.when(d < far)
        def _():
            each(z_copy(z, below(d), x), "wait_send")
            sent(above(d), False)
        return carry

    lax.fori_loop(1, far + 1, settle, 0)


def read_kernel(x_ref, r_ref, k_ref, v_ref, q_ref, cos_ref, sin_ref, plain_ref, value_ref, rot_ref, read_ref):
    spots, rope, span = r_ref.shape[1:]
    kw = k_ref.shape[1]
    for i in range(spots):
        rot_ref[0, :, i * span:(i + 1) * span] = r_ref[0, i]
    normed = x_ref[0]
    keys = jnp.dot(normed, k_ref[...], preferred_element_type=F32).astype(BF16)
    values = jnp.dot(normed, v_ref[...], preferred_element_type=F32).astype(BF16)
    plain_ref[0] = keys
    value_ref[0] = values
    part = pl.program_id(0)
    both = q_ref[...].astype(F32)
    query = jnp.where(part == 0, both[:1], both[1:])
    turned = turn(query[:, kw:], cos_ref[...], sin_ref[...]).astype(BF16)
    contract = (((1,), (1,)), ((), ()))
    scores = lax.dot_general(query[:, :kw].astype(BF16), keys, contract, preferred_element_type=F32)
    scores = scores + jnp.dot(turned, rot_ref[0], preferred_element_type=F32)
    scores = scores * (1.0 / (kw + rope) ** 0.5)
    weights = jnp.exp(scores - jnp.max(scores, axis=-1, keepdims=True))
    total = jnp.sum(weights, axis=-1, keepdims=True)
    mixed = jnp.dot(weights.astype(BF16), values, preferred_element_type=F32) / total
    spot = lax.broadcasted_iota(jnp.int32, read_ref.shape, 0)
    kept = jnp.where(spot == part, mixed, read_ref[...].astype(F32))
    read_ref[...] = jnp.where((part > 0) | (spot == 0), kept, 0.0).astype(BF16)


def body(planes, spots, tokens, latent_down, rope_weight, norm_scale, key_up, value_up, query):
    span = tokens.shape[1]
    rows, lat = latent_down.shape
    rope = rope_weight.shape[1]
    heads, kw = key_up.shape[1:]
    vw = value_up.shape[2]
    assert heads == 1
    length = spots * span
    cosine, sine = turn_tables(np.arange(length + 1), rope)
    vmem = pl.BlockSpec(memory_space=pltpu.VMEM)
    hbm = pl.BlockSpec(memory_space=pl.ANY)
    dma = pltpu.SemaphoreType.DMA
    x_all, rot_all = pl.pallas_call(
        functools.partial(move_kernel, planes, spots),
        out_shape=(jax.ShapeDtypeStruct((CORES, spots, span, lat), BF16),
                   jax.ShapeDtypeStruct((CORES, spots, rope, span), BF16)),
        in_specs=[hbm, hbm, hbm, vmem, hbm, hbm],
        out_specs=(vmem, vmem),
        scratch_shapes=[
            pltpu.VMEM((CORES, planes, span, rows), BF16),
            pltpu.VMEM((planes, rows, lat), BF16),
            pltpu.VMEM((planes, rope, rows), BF16),
            pltpu.VMEM((CORES * span, lat), F32),
            pltpu.VMEM((rope, CORES * span), F32),
            pltpu.VMEM((span, lat), F32),
            pltpu.VMEM((rope, span), F32),
            pltpu.VMEM((span, lat), BF16),
            pltpu.VMEM((rope, span), BF16),
            pltpu.VMEM((spots, span, lat), BF16),
            pltpu.VMEM((spots, rope, span), BF16),
            pltpu.VMEM((rope, span), F32),
            pltpu.VMEM((rope, span), F32),
            dma((planes,)), dma((planes,)), dma((planes + 4,)),
            dma((2, planes)), dma((2, planes)),
            dma((SIDE - 1, planes)), dma((SIDE - 1, planes)),
            dma((SIDE - 1, planes)), dma((SIDE - 1, planes)),
            dma((SIDE - 1, planes)), dma((SIDE - 1, planes)),
            dma((2,)), dma((2,)),
            dma((PARTS + 1,)), dma((PARTS + 1, SIDE)),
            dma((PARTS + 1, spots)), dma((PARTS + 1, spots)), dma((PARTS + 1, spots)),
            dma((PARTS + 1, spots)), dma((PARTS + 1, spots)),
            dma((PARTS + 1, spots)), dma((PARTS + 1, spots)),
        ],
        compiler_params=pltpu.CompilerParams(collective_id=0, has_side_effects=True),
    )(tokens, latent_down, rope_weight.T, norm_scale.reshape(1, lat),
      jnp.asarray(np.ascontiguousarray(cosine[:length].T)), jnp.asarray(np.ascontiguousarray(sine[:length].T)))
    x_all = x_all.reshape(CORES, length, lat)

    def whole(shape):
        return pl.BlockSpec(shape, lambda i: (0,) * len(shape))

    def per(shape):
        return pl.BlockSpec((1,) + shape, lambda i: (i,) + (0,) * len(shape))

    plain, value, rot, read = pl.pallas_call(
        read_kernel,
        grid=(CORES,),
        out_shape=(jax.ShapeDtypeStruct((CORES, length, kw), BF16),
                   jax.ShapeDtypeStruct((CORES, length, vw), BF16),
                   jax.ShapeDtypeStruct((CORES, rope, length), BF16),
                   jax.ShapeDtypeStruct((CORES, vw), BF16)),
        in_specs=[per((length, lat)), per((spots, rope, span)), whole((lat, kw)), whole((lat, vw)),
                  whole((CORES, query.shape[2])), whole((1, rope)), whole((1, rope))],
        out_specs=(per((length, kw)), per((length, vw)), per((rope, length)), whole((CORES, vw))),
    )(x_all, rot_all, key_up.reshape(lat, kw), value_up.reshape(lat, vw), query.reshape(CORES, -1),
      jnp.asarray(cosine[length:]), jnp.asarray(sine[length:]))
    return (plain.reshape(CORES, length, heads, kw), value.reshape(CORES, length, heads, vw), jnp.swapaxes(rot, 1, 2),
            read.reshape(CORES, heads, vw))


def solution(mesh):
    planes = mesh.shape["tp"] // CORES
    spots = mesh.shape["sp"]
    assert planes == spots == SIDE * SIDE
    in_specs = (
        P("tp", "sp", None),
        P("tp", None),
        P("tp", None),
        P(),
        P(None, "tp", None),
        P(None, "tp", None),
        P("sp", "tp", None),
    )
    out_specs = (
        P("sp", None, "tp", None),
        P("sp", None, "tp", None),
        P("sp", None, None),
        P("sp", "tp", None),
    )
    return jax.shard_map(functools.partial(body, planes, spots), mesh=mesh, in_specs=in_specs,
                         out_specs=out_specs, check_vma=False)
```

```python
import functools

import numpy as np
import jax
import jax.numpy as jnp
from jax import lax
from jax.sharding import PartitionSpec as P
from jax.experimental import pallas as pl
from jax.experimental.pallas import tpu as pltpu

CORES = 2
SIDE = 4
PARTS = 3
EARLY = 2
STEPS = 4
GRANT = 61_900_000
READ_GRANT = 40_000_000
BF16 = jnp.bfloat16
F32 = jnp.float32


def turn_tables(positions, width):
    half = width // 2
    freqs = (1.0 / np.float32(10000.0) ** (np.arange(half, dtype=np.float32) * np.float32(2.0) / np.float32(width))).astype(np.float32)
    angles = positions.astype(np.float32)[:, None] * freqs
    cosine = np.cos(angles).astype(np.float32)
    sine = np.sin(angles).astype(np.float32)
    return np.concatenate([cosine, cosine], -1), np.concatenate([-sine, sine], -1)


def turn(part, cosine, sine):
    half = part.shape[-1] // 2
    swapped = jnp.concatenate([part[:, half:], part[:, :half]], axis=-1)
    return part * cosine + swapped * sine


def move_kernel(planes, spots, tok, wl, wr, scale_hbm, cos_hbm, sin_hbm, kup, vup, q_hbm, qcos_hbm, qsin_hbm, fin, up, ask,
                tokens, wlat, wrope, acc, acct, other, othert, own, trans, cos_ref, sin_ref, scale, query, qcos, qsin,
                tok_s, tok_r, tok_o, own_s, z_s, z_r, a_s, a_r, b_s, b_r, t_s, t_r,
                acc_s, acc_r, x_s, x_r, up_s, down_s, in_r, y_s, y_r, p_s, p_r):
    s = lax.axis_index("sp")
    t = lax.axis_index("tp")
    z = t // CORES
    c = t % CORES
    x = s % SIDE
    y = s // SIDE
    rows, lat = wl.shape
    rope = wr.shape[0]
    span = tok.shape[1]
    rcut = rows // SIDE
    lcut = lat // SIDE
    pcut = rope // SIDE
    block = fin.shape[2]
    cut = block // PARTS
    kw = kup.shape[1]
    far = planes // 2

    def dev(yi, xi, zi, ci):
        return {"sp": yi * SIDE + xi, "tp": zi * CORES + ci}

    here = dev(y, x, z, 1 - c)

    def around(v, n):
        return lax.rem(v + n, n)

    def remote(src, dst, ss, rs, where):
        return pltpu.make_async_remote_copy(
            src_ref=src, dst_ref=dst, send_sem=ss, recv_sem=rs,
            device_id=where, device_id_type=pl.DeviceIdType.MESH)

    def each(copies, what):
        for p in copies:
            getattr(p, what)()

    def own_tok(u):
        cols = pl.ds(pl.multiple_of((u * CORES + c) * rows, 128), rows)
        return pltpu.make_async_copy(tok.at[0, :, cols], tokens.at[0, u], tok_o)

    def part_tok(u):
        cols = pl.ds(pl.multiple_of((u * CORES + 1 - c) * rows, 128), rows)
        return remote(tok.at[0, :, cols], tokens.at[1, u], tok_s, tok_r, here)

    own_wl = pltpu.make_async_copy(wl, wlat.at[z], own_s.at[0])
    own_wr = pltpu.make_async_copy(wr, wrope.at[z], own_s.at[1])
    place = pl.ds(pl.multiple_of(s * span, 128), span)
    tables = [pltpu.make_async_copy(cos_hbm.at[:, place], cos_ref, own_s.at[2]),
              pltpu.make_async_copy(sin_hbm.at[:, place], sin_ref, own_s.at[3]),
              pltpu.make_async_copy(scale_hbm, scale, own_s.at[4]),
              pltpu.make_async_copy(q_hbm, query, own_s.at[5]),
              pltpu.make_async_copy(qcos_hbm, qcos, own_s.at[6]),
              pltpu.make_async_copy(qsin_hbm, qsin, own_s.at[7]),
              pltpu.make_async_copy(kup, up.at[:, pl.ds(0, kw)], own_s.at[8]),
              pltpu.make_async_copy(vup, up.at[:, pl.ds(kw, up.shape[1] - kw)], own_s.at[9])]
    own_wl.start()
    own_wr.start()

    barrier = pltpu.get_barrier_semaphore()

    def greet(where):
        pl.semaphore_signal(barrier, inc=1, device_id=where, device_id_type=pl.DeviceIdType.MESH)

    for i in range(1, planes):
        greet(dev(y, x, around(z + i, planes), c))
    for i in range(1, SIDE):
        greet(dev(y, around(x + i, SIDE), z, c))
        greet(dev(around(y + i, SIDE), x, z, c))
    greet(here)
    for u in range(planes):
        own_tok(u).start()
    own_wl.wait()
    own_wr.wait()
    pl.semaphore_wait(barrier, planes - 1 + 2 * (SIDE - 1) + 1)

    def w_piece(u):
        return wlat.at[u, pl.ds(pl.multiple_of(y * rcut, 16), rcut), pl.ds(pl.multiple_of(x * lcut, 128), lcut)]

    def w_row(u):
        return wlat.at[u, pl.ds(pl.multiple_of(y * rcut, 16), rcut)]

    def w_col(u):
        return wlat.at[u, :, pl.ds(pl.multiple_of(x * lcut, 128), lcut)]

    def r_piece(u, i):
        return wrope.at[u, pl.ds(pl.multiple_of(i * pcut, 16), pcut)]

    def z_copy(u, zi, i):
        where = dev(y, x, zi, c)
        return [remote(w_piece(u), w_piece(u), z_s, z_r.at[u], where),
                remote(r_piece(u, i), r_piece(u, i), z_s, z_r.at[u], where)]

    def a_copy(u, o, by_row):
        where = dev(y, around(x + o, SIDE), z, c) if by_row else dev(around(y + o, SIDE), x, z, c)
        return remote(w_piece(u), w_piece(u), a_s, a_r.at[u], where)

    def b_copy(u, o, by_row):
        where = dev(around(y + o, SIDE), x, z, c) if by_row else dev(y, around(x + o, SIDE), z, c)
        part = w_row(u) if by_row else w_col(u)
        turned = r_piece(u, y if by_row else x)
        return [remote(part, part, b_s, b_r.at[u], where),
                remote(turned, turned, t_s, t_r.at[u], where)]

    def arrived(sem, count, deep, wide):
        part = wlat.at[pl.ds(0, count), pl.ds(0, deep), pl.ds(0, wide)]
        pltpu.make_async_copy(part, part, sem).wait()

    def below(d):
        return around(z - d, planes)

    def above(d):
        return around(z + d, planes)

    def z_send(d, carry):
        each(z_copy(z, above(d), y), "start")

        @pl.when(d < far)
        def _():
            each(z_copy(z, below(d), x), "start")
        return carry

    lax.fori_loop(1, far + 1, z_send, 0)
    for u in range(planes):
        part_tok(u).start()
    each(tables, "start")

    contract = (((1,), (1,)), ((), ()))

    def block_dot(u):
        v = tokens[:, u].reshape(CORES * span, rows)
        return (jnp.dot(v, wlat[u], preferred_element_type=F32),
                lax.dot_general(wrope[u], v, contract, preferred_element_type=F32))

    def own_block():
        pltpu.make_async_copy(tokens.at[0], tokens.at[0], tok_o).wait()
        pltpu.make_async_copy(tokens.at[1], tokens.at[1], tok_r).wait()
        a, b = block_dot(z)
        acc[...] = a
        acct[...] = b

    def first(u, by_row):
        arrived(z_r.at[u], 1, rcut + pcut, lcut)
        for o in range(1, SIDE):
            a_copy(u, o, by_row).start()

    def second(u, by_row):
        arrived(a_r.at[u], 1, rcut, lcut * (SIDE - 1))
        for o in range(1, SIDE):
            each(b_copy(u, o, by_row), "start")

    def third(u, by_row):
        arrived(b_r.at[u], 1, rcut * (SIDE - 1), lat)
        arrived(t_r.at[u], 1, pcut, rows * (SIDE - 1))
        a, b = block_dot(u)
        acc[...] += a
        acct[...] += b

    def both(d, what):
        @pl.when((d >= 1) & (d <= far))
        def _():
            what(below(d), True)

        @pl.when((d >= 1) & (d < far))
        def _():
            what(above(d), False)

    def step(i, carry):
        both(i, first)
        both(i - 2, second)

        @pl.when(i == 3)
        def _():
            own_block()

        both(i - 4, third)
        return carry

    lax.fori_loop(1, far + 5, step, 0)

    swaps = [remote(acc.at[pl.ds(span, span)], other, acc_s.at[0], acc_r.at[0], here),
             remote(acct.at[:, pl.ds(span, span)], othert, acc_s.at[1], acc_r.at[1], here)]
    each(swaps, "start")
    each(tables, "wait")
    asked = query[...].astype(F32)
    ask[...] = jnp.concatenate([asked[:, :kw], turn(asked[:, kw:], qcos[...], qsin[...])], axis=1).astype(BF16)
    each(swaps, "wait")
    latent = acc[:span] + other[...]
    ropes = acct[:, :span] + othert[...]
    scaled = latent * lax.rsqrt(jnp.mean(latent * latent, axis=-1, keepdims=True) + 1e-06)
    normed = (scaled * scale[...]).astype(BF16)
    swapped = jnp.concatenate([ropes[rope // 2:], ropes[:rope // 2]], axis=0)
    rotated = (ropes * cos_ref[...] + swapped * sin_ref[...]).astype(BF16)

    xq = z % SIDE
    kq = z // SIDE
    origin = x == xq

    folded = jnp.concatenate([rotated[i * pcut:(i + 1) * pcut] for i in range(SIDE)], axis=1)

    @pl.when(origin)
    def _():
        trans[kq * SIDE + x, :span] = normed
        trans[kq * SIDE + x, span:] = folded

    @pl.when(~origin)
    def _():
        own[:span] = normed
        own[span:] = folded

    def chunk(p):
        return pl.ds(p * cut, cut)

    def x_copy(xs, p):
        slot = kq * SIDE + xs
        return remote(own.at[chunk(p)], trans.at[slot, chunk(p)], x_s, x_r.at[p, xs], dev(y, xq, z, c))

    def z_move(slot, p, zi, sem):
        part = trans.at[slot, chunk(p)]
        return remote(part, part, sem, in_r.at[p, slot], dev(y, x, zi, c))

    def up_move(slot, p):
        return z_move(slot, p, around(z + 1, planes), up_s)

    def down_move(slot, p):
        return z_move(slot, p, around(z - 1, planes), down_s)

    def y_move(k, xs, p, place):
        return remote(trans.at[k * SIDE + xs, chunk(p)], fin.at[c, place, chunk(p)], y_s, y_r.at[p, place], dev(k, x, z, c))

    def p_from(src, place, p):
        return remote(src, fin.at[c, place, chunk(p)], p_s, p_r, here)

    def p_pass(place, p):
        return p_from(fin.at[c, place, chunk(p)], place, p)

    def p_keep(xs, p):
        slot = y * SIDE + xs
        return p_from(trans.at[slot, chunk(p)], slot, p)

    def goes_up(f, p):
        return f < far if p < EARLY else f < far - 1

    def goes_down(f, p):
        return f < far - 1 if p < EARLY else f < far

    def hand_over(k, xs, p):
        @pl.when(k != y)
        def _():
            y_move(k, xs, p, y * SIDE + xs).start()

        @pl.when(k == y)
        def _():
            slot = k * SIDE + xs
            p_keep(xs, p).start()
            fin[c, slot, p * cut:(p + 1) * cut] = trans[slot, p * cut:(p + 1) * cut]

    @pl.when(~origin)
    def _():
        for p in range(PARTS):
            x_copy(x, p).start()

    e = lax.rem(z - x + planes, SIDE)
    lower = jnp.where(e == 0, SIDE, e)
    upper = SIDE - e

    def ring(i, carry):
        ib = i - lower
        ia = i - upper
        db = lower + SIDE * (ib // SIDE)
        da = upper + SIDE * (ia // SIDE)
        kb = around(z - db, planes) // SIDE
        ka = around(z + da, planes) // SIDE
        xb = lax.rem(ib + SIDE, SIDE)
        xa = lax.rem(ia + SIDE, SIDE)
        for p in range(PARTS):
            @pl.when(origin & (i < SIDE))
            def _():
                xs = lax.rem(x + i, SIDE)
                slot = kq * SIDE + xs

                @pl.when(i > 0)
                def _():
                    x_copy(xs, p).wait_recv()
                up_move(slot, p).start()
                down_move(slot, p).start()
                hand_over(kq, xs, p)

            @pl.when((ib >= 0) & (ib < 2 * SIDE) & ((db < far) | (p < EARLY)))
            def _():
                slot = kb * SIDE + lax.rem(x + xb, SIDE)
                up_move(slot, p).wait_recv()

                @pl.when(goes_up(db, p))
                def _():
                    up_move(slot, p).start()
                hand_over(kb, lax.rem(x + xb, SIDE), p)

            @pl.when((ia >= 0) & (ia < 2 * SIDE) & ((da < far) | (p >= EARLY)))
            def _():
                slot = ka * SIDE + lax.rem(x + xa, SIDE)
                down_move(slot, p).wait_recv()

                @pl.when(goes_down(da, p))
                def _():
                    down_move(slot, p).start()
                hand_over(ka, lax.rem(x + xa, SIDE), p)
        return carry

    lax.fori_loop(0, 3 * SIDE, ring, 0)

    def pass_on(xs, carry):
        for p in range(PARTS):
            for o in range(1, SIDE):
                place = around(y + o, SIDE) * SIDE + xs
                y_move(y, xs, p, place).wait_recv()
                p_pass(place, p).start()
        return carry

    lax.fori_loop(0, SIDE, pass_on, 0)

    pltpu.make_async_copy(trans, trans, p_r).wait()
    pltpu.make_async_copy(trans, trans, p_s).wait()
    kept = trans.at[pl.ds(0, spots - SIDE)]
    pltpu.make_async_copy(kept, kept, y_s).wait()

    def swept(sem, short, cuts):
        whole = trans.at[pl.ds(0, 2 * SIDE)]
        less = trans.at[pl.ds(0, SIDE * (PARTS + cuts) // 2), pl.ds(0, 2 * cut)]

        @pl.when(short)
        def _():
            pltpu.make_async_copy(less, less, sem).wait()

        @pl.when(~short)
        def _():
            pltpu.make_async_copy(whole, whole, sem).wait()

    swept(up_s, e == SIDE - 1, EARLY)
    swept(down_s, e == 1, PARTS - EARLY)

    @pl.when(~origin)
    def _():
        pltpu.make_async_copy(own, own, x_s).wait()

    pltpu.make_async_copy(tokens.at[1], tokens.at[1], tok_s).wait()
    arrived(z_s, planes - 1, rcut + pcut, lcut)
    arrived(a_s, planes - 1, rcut, lcut * (SIDE - 1))
    arrived(b_s, planes - 1, rcut * (SIDE - 1), lat)
    arrived(t_s, planes - 1, pcut, rows * (SIDE - 1))


def read_kernel(steps, x_ref, up_ref, q_ref, plain_ref, value_ref, rot_ref, read_ref, held, scores):
    i = pl.program_id(0)
    part = i // steps
    step = lax.rem(i, steps)
    spots, block, lat = x_ref.shape[1:]
    kw = plain_ref.shape[2]
    span = rot_ref.shape[2] // (spots // steps)
    rope = rot_ref.shape[1]
    fold = block - span
    count = spots // steps
    chosen = jnp.where(part == 0, q_ref[:1].astype(F32), q_ref[1:].astype(F32)).astype(BF16)
    up = up_ref[...]
    contract = (((1,), (1,)), ((), ()))
    for n in range(count):
        spot = step * count + n
        both = jnp.dot(x_ref[part, spot, :span], up, preferred_element_type=F32)
        keys = both[:, :kw].astype(BF16)
        values = both[:, kw:].astype(BF16)
        plain_ref[0, n * span:(n + 1) * span] = keys
        value_ref[0, n * span:(n + 1) * span] = values
        held[pl.ds(pl.multiple_of(spot * span, span), span)] = values
        wide = x_ref[part, spot, span:]
        rotated = jnp.concatenate([wide[:, g * span:(g + 1) * span] for g in range(rope // fold)], axis=0)
        rot_ref[0, :, n * span:(n + 1) * span] = rotated
        score = lax.dot_general(chosen[:, :kw], keys, contract, preferred_element_type=F32)
        score = score + jnp.dot(chosen[:, kw:], rotated, preferred_element_type=F32)
        scores[pl.ds(spot, 1)] = score * (1.0 / (kw + rope) ** 0.5)

    @pl.when(step == steps - 1)
    def _():
        full = scores[...]
        weights = jnp.exp(full - jnp.max(full, keepdims=True))
        total = jnp.sum(weights, keepdims=True)
        rounded = weights.astype(BF16)
        mixed = jnp.zeros((1, value_ref.shape[2]), F32)
        for n in range(spots):
            mixed += jnp.dot(rounded[n:n + 1], held[n * span:(n + 1) * span], preferred_element_type=F32)
        mixed = mixed / total
        row = lax.broadcasted_iota(jnp.int32, read_ref.shape, 0)
        kept = jnp.where(row == part, mixed, read_ref[...].astype(F32))
        read_ref[...] = jnp.where((part > 0) | (row == 0), kept, 0.0).astype(BF16)


def body(planes, spots, tokens, latent_down, rope_weight, norm_scale, key_up, value_up, query):
    span = tokens.shape[1]
    rows, lat = latent_down.shape
    rope = rope_weight.shape[1]
    heads, kw = key_up.shape[1:]
    vw = value_up.shape[2]
    assert heads == 1
    length = spots * span
    block = span + rope * span // lat
    cosine, sine = turn_tables(np.arange(length + 1), rope)
    vmem = pl.BlockSpec(memory_space=pltpu.VMEM)
    hbm = pl.BlockSpec(memory_space=pl.ANY)
    dma = pltpu.SemaphoreType.DMA
    one = pltpu.SemaphoreType.DMA
    x_all, up, asked = pl.pallas_call(
        functools.partial(move_kernel, planes, spots),
        out_shape=(pltpu.VMEM((CORES, spots, block, lat), BF16),
                   pltpu.VMEM((lat, kw + vw), BF16),
                   pltpu.VMEM((CORES, kw + rope), BF16)),
        in_specs=[hbm] * 11,
        out_specs=(vmem, vmem, vmem),
        scratch_shapes=[
            pltpu.VMEM((CORES, planes, span, rows), BF16),
            pltpu.VMEM((planes, rows, lat), BF16),
            pltpu.VMEM((planes, rope, rows), BF16),
            pltpu.VMEM((CORES * span, lat), F32),
            pltpu.VMEM((rope, CORES * span), F32),
            pltpu.VMEM((span, lat), F32),
            pltpu.VMEM((rope, span), F32),
            pltpu.VMEM((block, lat), BF16),
            pltpu.VMEM((spots, block, lat), BF16),
            pltpu.VMEM((rope, span), F32),
            pltpu.VMEM((rope, span), F32),
            pltpu.VMEM((1, lat), F32),
            pltpu.VMEM((CORES, kw + rope), BF16),
            pltpu.VMEM((1, rope), F32),
            pltpu.VMEM((1, rope), F32),
            one, one, one, dma((10,)),
            one, dma((planes,)), one, dma((planes,)),
            one, dma((planes,)), one, dma((planes,)),
            dma((2,)), dma((2,)),
            one, dma((PARTS, SIDE)), one, one, dma((PARTS, spots)),
            one, dma((PARTS, spots)), one, one,
        ],
        compiler_params=pltpu.CompilerParams(collective_id=0, has_side_effects=True, vmem_limit_bytes=GRANT),
    )(tokens, latent_down, rope_weight.T, norm_scale.reshape(1, lat),
      jnp.asarray(np.ascontiguousarray(cosine[:length].T)), jnp.asarray(np.ascontiguousarray(sine[:length].T)),
      key_up.reshape(lat, kw), value_up.reshape(lat, vw), query.reshape(CORES, kw + rope),
      jnp.asarray(cosine[length:]), jnp.asarray(sine[length:]))

    def whole(shape):
        return pl.BlockSpec(shape, lambda i: (0,) * len(shape))

    wide = length // STEPS
    plain, value, rot, read = pl.pallas_call(
        functools.partial(read_kernel, STEPS),
        grid=(CORES * STEPS,),
        out_shape=(jax.ShapeDtypeStruct((CORES, length, kw), BF16),
                   jax.ShapeDtypeStruct((CORES, length, vw), BF16),
                   jax.ShapeDtypeStruct((CORES, rope, length), BF16),
                   jax.ShapeDtypeStruct((CORES, vw), BF16)),
        in_specs=[vmem, vmem, vmem],
        out_specs=(pl.BlockSpec((1, wide, kw), lambda i: (i // STEPS, i % STEPS, 0)),
                   pl.BlockSpec((1, wide, vw), lambda i: (i // STEPS, i % STEPS, 0)),
                   pl.BlockSpec((1, rope, wide), lambda i: (i // STEPS, 0, i % STEPS)), whole((CORES, vw))),
        scratch_shapes=[pltpu.VMEM((length, vw), BF16), pltpu.VMEM((spots, span), F32)],
        compiler_params=pltpu.CompilerParams(vmem_limit_bytes=READ_GRANT),
    )(x_all, up, asked)
    return (plain.reshape(CORES, length, heads, kw), value.reshape(CORES, length, heads, vw), jnp.swapaxes(rot, 1, 2),
            read.reshape(CORES, heads, vw))


def solution(mesh):
    planes = mesh.shape["tp"] // CORES
    spots = mesh.shape["sp"]
    assert planes == spots == SIDE * SIDE
    in_specs = (
        P("tp", "sp", None),
        P("tp", None),
        P("tp", None),
        P(),
        P(None, "tp", None),
        P(None, "tp", None),
        P("sp", "tp", None),
    )
    out_specs = (
        P("sp", None, "tp", None),
        P("sp", None, "tp", None),
        P("sp", None, None),
        P("sp", "tp", None),
    )
    return jax.shard_map(functools.partial(body, planes, spots), mesh=mesh, in_specs=in_specs,
                         out_specs=out_specs, check_vma=False)
```

```python
import functools

import numpy as np
import jax
import jax.numpy as jnp
from jax import lax
from jax.sharding import PartitionSpec as P
from jax.experimental import pallas as pl
from jax.experimental.pallas import tpu as pltpu

CORES = 2
SIDE = 4
PARTS = 3
EARLY = 2
NEAR = 1
LAG = 4
HUB = 4
GRANT = 61_900_000
READ_GRANT = 40_000_000
BF16 = jnp.bfloat16
F32 = jnp.float32


def turn_tables(positions, width):
    half = width // 2
    freqs = (1.0 / np.float32(10000.0) ** (np.arange(half, dtype=np.float32) * np.float32(2.0) / np.float32(width))).astype(np.float32)
    angles = positions.astype(np.float32)[:, None] * freqs
    cosine = np.cos(angles).astype(np.float32)
    sine = np.sin(angles).astype(np.float32)
    return np.concatenate([cosine, cosine], -1), np.concatenate([-sine, sine], -1)


def turn(part, cosine, sine):
    half = part.shape[-1] // 2
    swapped = jnp.concatenate([part[:, half:], part[:, :half]], axis=-1)
    return part * cosine + swapped * sine


def move_kernel(planes, spots, tok, wl, wr, scale_hbm, cos_hbm, sin_hbm, kup, vup, q_hbm, qcos_hbm, qsin_hbm, fin, up, ask,
                tokens, wlat, wrope, acc, acct, other, othert, own, trans, cos_ref, sin_ref, scale, query, qcos, qsin,
                tok_s, tok_r, tok_o, own_s, z_s, z_r, a_s, a_r, b_s, b_r, t_s, t_r,
                acc_s, acc_r, x_s, x_r, up_s, down_s, in_r, y_s, y_r, p_s, p_r):
    s = lax.axis_index("sp")
    t = lax.axis_index("tp")
    z = t // CORES
    c = t % CORES
    x = s % SIDE
    y = s // SIDE
    rows, lat = wl.shape
    rope = wr.shape[0]
    span = tok.shape[1]
    rcut = rows // SIDE
    lcut = lat // SIDE
    pcut = rope // SIDE
    block = fin.shape[2]
    cut = block // PARTS
    kw = kup.shape[1]
    far = planes // 2

    def dev(yi, xi, zi, ci):
        return {"sp": yi * SIDE + xi, "tp": zi * CORES + ci}

    here = dev(y, x, z, 1 - c)

    def around(v, n):
        return lax.rem(v + n, n)

    def remote(src, dst, ss, rs, where):
        return pltpu.make_async_remote_copy(
            src_ref=src, dst_ref=dst, send_sem=ss, recv_sem=rs,
            device_id=where, device_id_type=pl.DeviceIdType.MESH)

    def each(copies, what):
        for p in copies:
            getattr(p, what)()

    def own_tok(u):
        cols = pl.ds(pl.multiple_of((u * CORES + c) * rows, 128), rows)
        return pltpu.make_async_copy(tok.at[0, :, cols], tokens.at[0, u], tok_o)

    def part_tok(u):
        cols = pl.ds(pl.multiple_of((u * CORES + 1 - c) * rows, 128), rows)
        return remote(tok.at[0, :, cols], tokens.at[1, u], tok_s, tok_r, here)

    own_wl = pltpu.make_async_copy(wl, wlat.at[z], own_s.at[0])
    own_wr = pltpu.make_async_copy(wr, wrope.at[z], own_s.at[1])
    place = pl.ds(pl.multiple_of(s * span, 128), span)
    tables = [pltpu.make_async_copy(cos_hbm.at[:, place], cos_ref, own_s.at[2]),
              pltpu.make_async_copy(sin_hbm.at[:, place], sin_ref, own_s.at[3]),
              pltpu.make_async_copy(scale_hbm, scale, own_s.at[4]),
              pltpu.make_async_copy(q_hbm, query, own_s.at[5]),
              pltpu.make_async_copy(qcos_hbm, qcos, own_s.at[6]),
              pltpu.make_async_copy(qsin_hbm, qsin, own_s.at[7]),
              pltpu.make_async_copy(kup, up.at[:, pl.ds(0, kw)], own_s.at[8]),
              pltpu.make_async_copy(vup, up.at[:, pl.ds(kw, up.shape[1] - kw)], own_s.at[9])]
    own_wl.start()
    own_wr.start()

    barrier = pltpu.get_barrier_semaphore()

    def greet(where):
        pl.semaphore_signal(barrier, inc=1, device_id=where, device_id_type=pl.DeviceIdType.MESH)

    for i in range(1, planes):
        greet(dev(y, x, around(z + i, planes), c))
    for i in range(1, SIDE):
        greet(dev(y, around(x + i, SIDE), z, c))
        greet(dev(around(y + i, SIDE), x, z, c))
    greet(here)
    for u in range(planes):
        own_tok(u).start()
    own_wl.wait()
    own_wr.wait()
    pl.semaphore_wait(barrier, planes - 1 + 2 * (SIDE - 1) + 1)

    def w_piece(u):
        return wlat.at[u, pl.ds(pl.multiple_of(y * rcut, 16), rcut), pl.ds(pl.multiple_of(x * lcut, 128), lcut)]

    def w_row(u):
        return wlat.at[u, pl.ds(pl.multiple_of(y * rcut, 16), rcut)]

    def w_col(u):
        return wlat.at[u, :, pl.ds(pl.multiple_of(x * lcut, 128), lcut)]

    def r_piece(u, i):
        return wrope.at[u, pl.ds(pl.multiple_of(i * pcut, 16), pcut)]

    def z_copy(u, zi, by_row, near):
        where = dev(y, x, zi, c)
        part = (w_row(u) if by_row else w_col(u)) if near else w_piece(u)
        turned = r_piece(u, y if by_row else x)
        return [remote(part, part, z_s, z_r.at[u], where), remote(turned, turned, z_s, z_r.at[u], where)]

    def a_copy(u, o, by_row):
        where = dev(y, around(x + o, SIDE), z, c) if by_row else dev(around(y + o, SIDE), x, z, c)
        return remote(w_piece(u), w_piece(u), a_s, a_r.at[u], where)

    def b_copy(u, o, by_row):
        where = dev(around(y + o, SIDE), x, z, c) if by_row else dev(y, around(x + o, SIDE), z, c)
        part = w_row(u) if by_row else w_col(u)
        turned = r_piece(u, y if by_row else x)
        return [remote(part, part, b_s, b_r.at[u], where),
                remote(turned, turned, t_s, t_r.at[u], where)]

    def arrived(sem, count, deep, wide):
        part = wlat.at[pl.ds(0, count), pl.ds(0, deep), pl.ds(0, wide)]
        pltpu.make_async_copy(part, part, sem).wait()

    def below(d):
        return around(z - d, planes)

    def above(d):
        return around(z + d, planes)

    for d in range(1, NEAR + 1):
        each(z_copy(z, above(d), True, True), "start")
        each(z_copy(z, below(d), False, True), "start")

    for d in range(NEAR + 1, HUB + 1):
        each(z_copy(z, above(d), True, False), "start")
        each(z_copy(z, below(d), False, False), "start")

    for u in range(planes):
        part_tok(u).start()
    each(tables, "start")

    contract = (((1,), (1,)), ((), ()))

    def block_dot(u):
        v = tokens[:, u].reshape(CORES * span, rows)
        return (jnp.dot(v, wlat[u], preferred_element_type=F32),
                lax.dot_general(wrope[u], v, contract, preferred_element_type=F32))

    def own_block():
        pltpu.make_async_copy(tokens.at[0], tokens.at[0], tok_o).wait()
        pltpu.make_async_copy(tokens.at[1], tokens.at[1], tok_r).wait()
        a, b = block_dot(z)
        acc[...] = a
        acct[...] = b

    def spread(u, by_row):
        for o in range(1, SIDE):
            a_copy(u, o, by_row).start()

    def first(u, by_row):
        arrived(z_r.at[u], 1, rcut + pcut, lcut)
        spread(u, by_row)

    def second(u, by_row):
        arrived(a_r.at[u], 1, rcut, lcut * (SIDE - 1))
        for o in range(1, SIDE):
            each(b_copy(u, o, by_row), "start")

    def nearby(u, by_row):
        arrived(z_r.at[u], 1, rcut + pcut, lcut * (SIDE - 1))
        for o in range(1, SIDE):
            each(b_copy(u, o, by_row), "start")

    def third(u, by_row):
        arrived(b_r.at[u], 1, rcut * (SIDE - 1), lat)
        arrived(t_r.at[u], 1, pcut, rows * (SIDE - 1))
        a, b = block_dot(u)
        acc[...] += a
        acct[...] += b

    def both(d, low, what):
        @pl.when((d >= low) & (d <= far))
        def _():
            what(below(d), True)

        @pl.when((d >= low) & (d < far))
        def _():
            what(above(d), False)

    for d in range(1, NEAR + 1):
        nearby(below(d), True)
        nearby(above(d), False)

    arrived(z_r.at[below(HUB)], 1, rcut + pcut, lcut)
    for d in range(1, far - HUB + 1):
        each(z_copy(below(HUB), above(d), True, False), "start")
    arrived(z_r.at[above(HUB)], 1, rcut + pcut, lcut)
    for d in range(1, far - HUB):
        each(z_copy(above(HUB), below(d), False, False), "start")
    spread(below(HUB), True)
    spread(above(HUB), False)
    for d in range(NEAR + 1, HUB):
        first(below(d), True)
        first(above(d), False)

    def step(i, carry):
        both(i + HUB - NEAR, HUB + 1, first)

        @pl.when(i == NEAR + 1)
        def _():
            own_block()

        both(i, NEAR + 1, second)
        both(i - LAG, 1, third)
        return carry

    lax.fori_loop(NEAR + 1, far + LAG + 1, step, 0)

    swaps = [remote(acc.at[pl.ds(span, span)], other, acc_s.at[0], acc_r.at[0], here),
             remote(acct.at[:, pl.ds(span, span)], othert, acc_s.at[1], acc_r.at[1], here)]
    each(swaps, "start")
    each(tables, "wait")
    asked = query[...].astype(F32)
    ask[...] = jnp.concatenate([asked[:, :kw], turn(asked[:, kw:], qcos[...], qsin[...])], axis=1).astype(BF16)
    each(swaps, "wait")
    latent = acc[:span] + other[...]
    ropes = acct[:, :span] + othert[...]
    scaled = latent * lax.rsqrt(jnp.mean(latent * latent, axis=-1, keepdims=True) + 1e-06)
    normed = (scaled * scale[...]).astype(BF16)
    swapped = jnp.concatenate([ropes[rope // 2:], ropes[:rope // 2]], axis=0)
    rotated = (ropes * cos_ref[...] + swapped * sin_ref[...]).astype(BF16)

    xq = z % SIDE
    kq = z // SIDE
    origin = x == xq

    folded = jnp.concatenate([rotated[i * pcut:(i + 1) * pcut] for i in range(SIDE)], axis=1)

    @pl.when(origin)
    def _():
        trans[kq * SIDE + x, :span] = normed
        trans[kq * SIDE + x, span:] = folded

    @pl.when(~origin)
    def _():
        own[:span] = normed
        own[span:] = folded

    def chunk(p):
        return pl.ds(p * cut, cut)

    def x_copy(xs, p):
        slot = kq * SIDE + xs
        return remote(own.at[chunk(p)], trans.at[slot, chunk(p)], x_s, x_r.at[p, xs], dev(y, xq, z, c))

    def z_move(slot, p, zi, sem):
        part = trans.at[slot, chunk(p)]
        return remote(part, part, sem, in_r.at[p, slot], dev(y, x, zi, c))

    def up_move(slot, p):
        return z_move(slot, p, around(z + 1, planes), up_s)

    def down_move(slot, p):
        return z_move(slot, p, around(z - 1, planes), down_s)

    def y_move(k, xs, p, place):
        return remote(trans.at[k * SIDE + xs, chunk(p)], fin.at[c, place, chunk(p)], y_s, y_r.at[p, place], dev(k, x, z, c))

    def p_from(src, place, p):
        return remote(src, fin.at[c, place, chunk(p)], p_s, p_r, here)

    def p_pass(place, p):
        return p_from(fin.at[c, place, chunk(p)], place, p)

    def p_keep(xs, p):
        slot = y * SIDE + xs
        return p_from(trans.at[slot, chunk(p)], slot, p)

    def goes_up(f, p):
        return f < far if p < EARLY else f < far - 1

    def goes_down(f, p):
        return f < far - 1 if p < EARLY else f < far

    def hand_over(k, xs, p):
        @pl.when(k != y)
        def _():
            y_move(k, xs, p, y * SIDE + xs).start()

        @pl.when(k == y)
        def _():
            slot = k * SIDE + xs
            p_keep(xs, p).start()
            fin[c, slot, p * cut:(p + 1) * cut] = trans[slot, p * cut:(p + 1) * cut]

    @pl.when(~origin)
    def _():
        for p in range(PARTS):
            x_copy(x, p).start()

    e = lax.rem(z - x + planes, SIDE)
    lower = jnp.where(e == 0, SIDE, e)
    upper = SIDE - e

    def ring(i, carry):
        ib = i - lower
        ia = i - upper
        db = lower + SIDE * (ib // SIDE)
        da = upper + SIDE * (ia // SIDE)
        kb = around(z - db, planes) // SIDE
        ka = around(z + da, planes) // SIDE
        xb = lax.rem(ib + SIDE, SIDE)
        xa = lax.rem(ia + SIDE, SIDE)
        for p in range(PARTS):
            @pl.when(origin & (i < SIDE))
            def _():
                xs = lax.rem(x + i, SIDE)
                slot = kq * SIDE + xs

                @pl.when(i > 0)
                def _():
                    x_copy(xs, p).wait_recv()
                up_move(slot, p).start()
                down_move(slot, p).start()
                hand_over(kq, xs, p)

            @pl.when((ib >= 0) & (ib < 2 * SIDE) & ((db < far) | (p < EARLY)))
            def _():
                slot = kb * SIDE + lax.rem(x + xb, SIDE)
                up_move(slot, p).wait_recv()

                @pl.when(goes_up(db, p))
                def _():
                    up_move(slot, p).start()
                hand_over(kb, lax.rem(x + xb, SIDE), p)

            @pl.when((ia >= 0) & (ia < 2 * SIDE) & ((da < far) | (p >= EARLY)))
            def _():
                slot = ka * SIDE + lax.rem(x + xa, SIDE)
                down_move(slot, p).wait_recv()

                @pl.when(goes_down(da, p))
                def _():
                    down_move(slot, p).start()
                hand_over(ka, lax.rem(x + xa, SIDE), p)
        return carry

    lax.fori_loop(0, 3 * SIDE, ring, 0)

    def pass_on(xs, carry):
        for p in range(PARTS):
            for o in range(1, SIDE):
                place = around(y + o, SIDE) * SIDE + xs
                y_move(y, xs, p, place).wait_recv()
                p_pass(place, p).start()
        return carry

    lax.fori_loop(0, SIDE, pass_on, 0)

    pltpu.make_async_copy(trans, trans, p_r).wait()
    pltpu.make_async_copy(trans, trans, p_s).wait()
    kept = trans.at[pl.ds(0, spots - SIDE)]
    pltpu.make_async_copy(kept, kept, y_s).wait()

    def swept(sem, short, cuts):
        whole = trans.at[pl.ds(0, 2 * SIDE)]
        less = trans.at[pl.ds(0, SIDE * (PARTS + cuts) // 2), pl.ds(0, 2 * cut)]

        @pl.when(short)
        def _():
            pltpu.make_async_copy(less, less, sem).wait()

        @pl.when(~short)
        def _():
            pltpu.make_async_copy(whole, whole, sem).wait()

    swept(up_s, e == SIDE - 1, EARLY)
    swept(down_s, e == 1, PARTS - EARLY)

    @pl.when(~origin)
    def _():
        pltpu.make_async_copy(own, own, x_s).wait()

    pltpu.make_async_copy(tokens.at[1], tokens.at[1], tok_s).wait()
    arrived(z_s, planes - 1 - 2 * NEAR, rcut + pcut, lcut)
    arrived(z_s, 2 * NEAR, rcut + pcut, lcut * (SIDE - 1))
    arrived(a_s, planes - 1 - 2 * NEAR, rcut, lcut * (SIDE - 1))
    arrived(b_s, planes - 1, rcut * (SIDE - 1), lat)
    arrived(t_s, planes - 1, pcut, rows * (SIDE - 1))


def read_kernel(x_ref, up_ref, q_ref, plain_ref, value_ref, rot_ref, read_ref):
    part = pl.program_id(0)
    spots, block, lat = x_ref.shape[1:]
    length, kw = plain_ref.shape[1:]
    rope = rot_ref.shape[1]
    span = length // spots
    fold = block - span
    wide = x_ref[part, :, span:]
    for g in range(rope // fold):
        for n in range(spots):
            rot_ref[0, g * fold:(g + 1) * fold, n * span:(n + 1) * span] = wide[n, :, g * span:(g + 1) * span]
    both = jnp.dot(x_ref[part, :, :span].reshape(length, lat), up_ref[...], preferred_element_type=F32).astype(BF16)
    keys = both[:, :kw]
    values = both[:, kw:]
    plain_ref[0] = keys
    value_ref[0] = values
    chosen = jnp.where(part == 0, q_ref[:1].astype(F32), q_ref[1:].astype(F32)).astype(BF16)
    contract = (((1,), (1,)), ((), ()))
    scores = lax.dot_general(chosen[:, :kw], keys, contract, preferred_element_type=F32)
    scores = scores + jnp.dot(chosen[:, kw:], rot_ref[0], preferred_element_type=F32)
    scores = scores * (1.0 / (kw + rope) ** 0.5)
    weights = jnp.exp(scores - jnp.max(scores, axis=-1, keepdims=True))
    total = jnp.sum(weights, axis=-1, keepdims=True)
    mixed = jnp.dot(weights.astype(BF16), values, preferred_element_type=F32) / total
    row = lax.broadcasted_iota(jnp.int32, read_ref.shape, 0)
    kept = jnp.where(row == part, mixed, read_ref[...].astype(F32))
    read_ref[...] = jnp.where((part > 0) | (row == 0), kept, 0.0).astype(BF16)


def body(planes, spots, tokens, latent_down, rope_weight, norm_scale, key_up, value_up, query):
    span = tokens.shape[1]
    rows, lat = latent_down.shape
    rope = rope_weight.shape[1]
    heads, kw = key_up.shape[1:]
    vw = value_up.shape[2]
    assert heads == 1
    length = spots * span
    block = span + rope * span // lat
    cosine, sine = turn_tables(np.arange(length + 1), rope)
    vmem = pl.BlockSpec(memory_space=pltpu.VMEM)
    hbm = pl.BlockSpec(memory_space=pl.ANY)
    dma = pltpu.SemaphoreType.DMA
    one = pltpu.SemaphoreType.DMA
    x_all, up, asked = pl.pallas_call(
        functools.partial(move_kernel, planes, spots),
        out_shape=(pltpu.VMEM((CORES, spots, block, lat), BF16),
                   pltpu.VMEM((lat, kw + vw), BF16),
                   pltpu.VMEM((CORES, kw + rope), BF16)),
        in_specs=[hbm] * 11,
        out_specs=(vmem, vmem, vmem),
        scratch_shapes=[
            pltpu.VMEM((CORES, planes, span, rows), BF16),
            pltpu.VMEM((planes, rows, lat), BF16),
            pltpu.VMEM((planes, rope, rows), BF16),
            pltpu.VMEM((CORES * span, lat), F32),
            pltpu.VMEM((rope, CORES * span), F32),
            pltpu.VMEM((span, lat), F32),
            pltpu.VMEM((rope, span), F32),
            pltpu.VMEM((block, lat), BF16),
            pltpu.VMEM((spots, block, lat), BF16),
            pltpu.VMEM((rope, span), F32),
            pltpu.VMEM((rope, span), F32),
            pltpu.VMEM((1, lat), F32),
            pltpu.VMEM((CORES, kw + rope), BF16),
            pltpu.VMEM((1, rope), F32),
            pltpu.VMEM((1, rope), F32),
            one, one, one, dma((10,)),
            one, dma((planes,)), one, dma((planes,)),
            one, dma((planes,)), one, dma((planes,)),
            dma((2,)), dma((2,)),
            one, dma((PARTS, SIDE)), one, one, dma((PARTS, spots)),
            one, dma((PARTS, spots)), one, one,
        ],
        compiler_params=pltpu.CompilerParams(collective_id=0, has_side_effects=True, vmem_limit_bytes=GRANT),
    )(tokens, latent_down, rope_weight.T, norm_scale.reshape(1, lat),
      jnp.asarray(np.ascontiguousarray(cosine[:length].T)), jnp.asarray(np.ascontiguousarray(sine[:length].T)),
      key_up.reshape(lat, kw), value_up.reshape(lat, vw), query.reshape(CORES, kw + rope),
      jnp.asarray(cosine[length:]), jnp.asarray(sine[length:]))

    def whole(shape):
        return pl.BlockSpec(shape, lambda i: (0,) * len(shape))

    def per(shape):
        return pl.BlockSpec((1,) + shape, lambda i: (i,) + (0,) * len(shape))

    plain, value, rot, read = pl.pallas_call(
        read_kernel,
        grid=(CORES,),
        out_shape=(jax.ShapeDtypeStruct((CORES, length, kw), BF16),
                   jax.ShapeDtypeStruct((CORES, length, vw), BF16),
                   jax.ShapeDtypeStruct((CORES, rope, length), BF16),
                   jax.ShapeDtypeStruct((CORES, vw), BF16)),
        in_specs=[vmem, vmem, vmem],
        out_specs=(per((length, kw)), per((length, vw)), per((rope, length)), whole((CORES, vw))),
        compiler_params=pltpu.CompilerParams(vmem_limit_bytes=READ_GRANT),
    )(x_all, up, asked)
    return (plain.reshape(CORES, length, heads, kw), value.reshape(CORES, length, heads, vw), jnp.swapaxes(rot, 1, 2),
            read.reshape(CORES, heads, vw))


def solution(mesh):
    planes = mesh.shape["tp"] // CORES
    spots = mesh.shape["sp"]
    assert planes == spots == SIDE * SIDE
    in_specs = (
        P("tp", "sp", None),
        P("tp", None),
        P("tp", None),
        P(),
        P(None, "tp", None),
        P(None, "tp", None),
        P("sp", "tp", None),
    )
    out_specs = (
        P("sp", None, "tp", None),
        P("sp", None, "tp", None),
        P("sp", None, None),
        P("sp", "tp", None),
    )
    return jax.shard_map(functools.partial(body, planes, spots), mesh=mesh, in_specs=in_specs,
                         out_specs=out_specs, check_vma=False)
```

```python
import functools

import numpy as np
import jax
import jax.numpy as jnp
from jax import lax
from jax.sharding import PartitionSpec as P
from jax.experimental import pallas as pl
from jax.experimental.pallas import tpu as pltpu

CORES = 2
SIDE = 4
PARTS = 3
EARLY = 2
NEAR = 1
LAG = 5
HUB = 4
GRANT = 61_900_000
READ_GRANT = 40_000_000
BF16 = jnp.bfloat16
F32 = jnp.float32


def turn_tables(positions, width):
    half = width // 2
    freqs = (1.0 / np.float32(10000.0) ** (np.arange(half, dtype=np.float32) * np.float32(2.0) / np.float32(width))).astype(np.float32)
    angles = positions.astype(np.float32)[:, None] * freqs
    cosine = np.cos(angles).astype(np.float32)
    sine = np.sin(angles).astype(np.float32)
    return np.concatenate([cosine, cosine], -1), np.concatenate([-sine, sine], -1)


def turn(part, cosine, sine):
    half = part.shape[-1] // 2
    swapped = jnp.concatenate([part[:, half:], part[:, :half]], axis=-1)
    return part * cosine + swapped * sine


def move_kernel(planes, spots, tok, wl, wr, scale_hbm, cos_hbm, sin_hbm, kup, vup, q_hbm, qcos_hbm, qsin_hbm, fin, up, ask,
                tokens, wlat, wrope, acc, acct, other, othert, own, trans, cos_ref, sin_ref, scale, query, qcos, qsin,
                tok_s, tok_r, tok_o, own_s, z_s, z_r, a_s, a_r, b_s, b_r,
                acc_s, acc_r, x_s, x_r, up_s, down_s, in_r, y_s, y_r, p_s, p_r):
    s = lax.axis_index("sp")
    t = lax.axis_index("tp")
    z = t // CORES
    c = t % CORES
    x = s % SIDE
    y = s // SIDE
    rows, lat = wl.shape
    rope = wr.shape[0]
    span = tok.shape[1]
    rcut = rows // SIDE
    lcut = lat // SIDE
    pcut = rope // SIDE
    block = fin.shape[2]
    cut = block // PARTS
    kw = kup.shape[1]
    far = planes // 2

    def dev(yi, xi, zi, ci):
        return {"sp": yi * SIDE + xi, "tp": zi * CORES + ci}

    here = dev(y, x, z, 1 - c)

    def around(v, n):
        return lax.rem(v + n, n)

    def remote(src, dst, ss, rs, where):
        return pltpu.make_async_remote_copy(
            src_ref=src, dst_ref=dst, send_sem=ss, recv_sem=rs,
            device_id=where, device_id_type=pl.DeviceIdType.MESH)

    def each(copies, what):
        for p in copies:
            getattr(p, what)()

    def own_tok(u):
        cols = pl.ds(pl.multiple_of((u * CORES + c) * rows, 128), rows)
        return pltpu.make_async_copy(tok.at[0, :, cols], tokens.at[0, u], tok_o)

    def part_tok(u):
        cols = pl.ds(pl.multiple_of((u * CORES + 1 - c) * rows, 128), rows)
        return remote(tok.at[0, :, cols], tokens.at[1, u], tok_s, tok_r, here)

    own_wl = pltpu.make_async_copy(wl, wlat.at[z], own_s.at[0])
    own_wr = pltpu.make_async_copy(wr, wrope.at[z], own_s.at[1])
    place = pl.ds(pl.multiple_of(s * span, 128), span)
    tables = [pltpu.make_async_copy(cos_hbm.at[:, place], cos_ref, own_s.at[2]),
              pltpu.make_async_copy(sin_hbm.at[:, place], sin_ref, own_s.at[3]),
              pltpu.make_async_copy(scale_hbm, scale, own_s.at[4]),
              pltpu.make_async_copy(q_hbm, query, own_s.at[5]),
              pltpu.make_async_copy(qcos_hbm, qcos, own_s.at[6]),
              pltpu.make_async_copy(qsin_hbm, qsin, own_s.at[7]),
              pltpu.make_async_copy(kup, up.at[:, pl.ds(0, kw)], own_s.at[8]),
              pltpu.make_async_copy(vup, up.at[:, pl.ds(kw, up.shape[1] - kw)], own_s.at[9])]
    own_wl.start()
    own_wr.start()

    barrier = pltpu.get_barrier_semaphore()

    def greet(where):
        pl.semaphore_signal(barrier, inc=1, device_id=where, device_id_type=pl.DeviceIdType.MESH)

    for i in range(1, planes):
        greet(dev(y, x, around(z + i, planes), c))
    for i in range(1, SIDE):
        greet(dev(y, around(x + i, SIDE), z, c))
        greet(dev(around(y + i, SIDE), x, z, c))
    greet(here)
    for u in range(planes):
        own_tok(u).start()
    own_wl.wait()
    own_wr.wait()
    pl.semaphore_wait(barrier, planes - 1 + 2 * (SIDE - 1) + 1)

    def w_piece(u):
        return wlat.at[u, pl.ds(pl.multiple_of(y * rcut, 16), rcut), pl.ds(pl.multiple_of(x * lcut, 128), lcut)]

    def w_row(u):
        return wlat.at[u, pl.ds(pl.multiple_of(y * rcut, 16), rcut)]

    def w_col(u):
        return wlat.at[u, :, pl.ds(pl.multiple_of(x * lcut, 128), lcut)]

    def r_piece(u, i):
        return wrope.at[u, pl.ds(pl.multiple_of(i * pcut, 16), pcut)]

    def z_copy(u, zi, by_row, near):
        where = dev(y, x, zi, c)
        part = (w_row(u) if by_row else w_col(u)) if near else w_piece(u)
        turned = r_piece(u, y if by_row else x)
        return [remote(part, part, z_s, z_r.at[u], where), remote(turned, turned, z_s, z_r.at[u], where)]

    def a_copy(u, o, by_row):
        where = dev(y, around(x + o, SIDE), z, c) if by_row else dev(around(y + o, SIDE), x, z, c)
        return remote(w_piece(u), w_piece(u), a_s, a_r.at[u], where)

    def b_copy(u, o, by_row):
        where = dev(around(y + o, SIDE), x, z, c) if by_row else dev(y, around(x + o, SIDE), z, c)
        part = w_row(u) if by_row else w_col(u)
        turned = r_piece(u, y if by_row else x)
        return [remote(part, part, b_s, b_r.at[u], where),
                remote(turned, turned, b_s, b_r.at[u], where)]

    def arrived(sem, count, deep, wide):
        part = wlat.at[pl.ds(0, count), pl.ds(0, deep), pl.ds(0, wide)]
        pltpu.make_async_copy(part, part, sem).wait()

    def below(d):
        return around(z - d, planes)

    def above(d):
        return around(z + d, planes)

    for d in range(HUB, 0, -1):
        each(z_copy(z, above(d), True, d <= NEAR), "start")
        each(z_copy(z, below(d), False, d <= NEAR), "start")

    for u in range(planes):
        part_tok(u).start()
    each(tables, "start")

    contract = (((1,), (1,)), ((), ()))

    def block_dot(u):
        v = tokens[:, u].reshape(CORES * span, rows)
        return (jnp.dot(v, wlat[u], preferred_element_type=F32),
                lax.dot_general(wrope[u], v, contract, preferred_element_type=F32))

    def own_block():
        pltpu.make_async_copy(tokens.at[0], tokens.at[0], tok_o).wait()
        pltpu.make_async_copy(tokens.at[1], tokens.at[1], tok_r).wait()
        a, b = block_dot(z)
        acc[...] = a
        acct[...] = b

    def spread(u, by_row):
        for o in range(1, SIDE):
            a_copy(u, o, by_row).start()

    def first(u, by_row):
        arrived(z_r.at[u], 1, rcut + pcut, lcut)
        spread(u, by_row)

    def second(u, by_row):
        arrived(a_r.at[u], 1, rcut, lcut * (SIDE - 1))
        for o in range(1, SIDE):
            each(b_copy(u, o, by_row), "start")

    def nearby(u, by_row):
        arrived(z_r.at[u], 1, rcut + pcut, lcut * (SIDE - 1))
        for o in range(1, SIDE):
            each(b_copy(u, o, by_row), "start")

    def third(u, by_row):
        arrived(b_r.at[u], (SIDE - 1) * (SIDE - 1), rcut + pcut, lcut)
        a, b = block_dot(u)
        acc[...] += a
        acct[...] += b

    def both(d, low, what):
        @pl.when((d >= low) & (d <= far))
        def _():
            what(below(d), True)

        @pl.when((d >= low) & (d < far))
        def _():
            what(above(d), False)

    for d in range(1, NEAR + 1):
        nearby(below(d), True)
        nearby(above(d), False)

    arrived(z_r.at[below(HUB)], 1, rcut + pcut, lcut)
    for d in range(1, far - HUB + 1):
        each(z_copy(below(HUB), above(d), True, False), "start")
    arrived(z_r.at[above(HUB)], 1, rcut + pcut, lcut)
    for d in range(1, far - HUB):
        each(z_copy(above(HUB), below(d), False, False), "start")
    spread(below(HUB), True)
    spread(above(HUB), False)
    for d in range(NEAR + 1, HUB):
        first(below(d), True)
        first(above(d), False)

    def step(i, carry):
        both(i + HUB - NEAR, HUB + 1, first)

        @pl.when(i == NEAR + 1)
        def _():
            own_block()

        both(i, NEAR + 1, second)
        both(i - LAG, 1, third)
        return carry

    lax.fori_loop(NEAR + 1, far + LAG + 1, step, 0)

    swaps = [remote(acc.at[pl.ds(span, span)], other, acc_s.at[0], acc_r.at[0], here),
             remote(acct.at[:, pl.ds(span, span)], othert, acc_s.at[1], acc_r.at[1], here)]
    each(swaps, "start")
    each(tables, "wait")
    asked = query[...].astype(F32)
    ask[...] = jnp.concatenate([asked[:, :kw], turn(asked[:, kw:], qcos[...], qsin[...])], axis=1).astype(BF16)
    each(swaps, "wait")
    latent = acc[:span] + other[...]
    ropes = acct[:, :span] + othert[...]
    scaled = latent * lax.rsqrt(jnp.mean(latent * latent, axis=-1, keepdims=True) + 1e-06)
    normed = (scaled * scale[...]).astype(BF16)
    swapped = jnp.concatenate([ropes[rope // 2:], ropes[:rope // 2]], axis=0)
    rotated = (ropes * cos_ref[...] + swapped * sin_ref[...]).astype(BF16)

    xq = z % SIDE
    kq = z // SIDE
    origin = x == xq

    folded = jnp.concatenate([rotated[i * pcut:(i + 1) * pcut] for i in range(SIDE)], axis=1)

    @pl.when(origin)
    def _():
        trans[kq * SIDE + x, :span] = normed
        trans[kq * SIDE + x, span:] = folded

    @pl.when(~origin)
    def _():
        own[:span] = normed
        own[span:] = folded

    def chunk(p):
        return pl.ds(p * cut, cut)

    def x_copy(xs, p):
        slot = kq * SIDE + xs
        return remote(own.at[chunk(p)], trans.at[slot, chunk(p)], x_s, x_r.at[p, xs], dev(y, xq, z, c))

    def z_move(slot, p, zi, sem):
        part = trans.at[slot, chunk(p)]
        return remote(part, part, sem, in_r.at[p, slot], dev(y, x, zi, c))

    def up_move(slot, p):
        return z_move(slot, p, around(z + 1, planes), up_s)

    def down_move(slot, p):
        return z_move(slot, p, around(z - 1, planes), down_s)

    def y_move(k, xs, p, place):
        return remote(trans.at[k * SIDE + xs, chunk(p)], fin.at[c, place, chunk(p)], y_s, y_r.at[place], dev(k, x, z, c))

    def p_from(src, place, p):
        return remote(src, fin.at[c, place, chunk(p)], p_s, p_r, here)

    def p_keep(xs, p):
        slot = y * SIDE + xs
        return p_from(trans.at[slot, chunk(p)], slot, p)

    def goes_up(f, p):
        return f < far if p < EARLY else f < far - 1

    def goes_down(f, p):
        return f < far - 1 if p < EARLY else f < far

    def hand_over(k, xs, p):
        @pl.when(k != y)
        def _():
            y_move(k, xs, p, y * SIDE + xs).start()

        @pl.when(k == y)
        def _():
            slot = k * SIDE + xs
            p_keep(xs, p).start()
            fin[c, slot, p * cut:(p + 1) * cut] = trans[slot, p * cut:(p + 1) * cut]

    @pl.when(~origin)
    def _():
        for p in range(PARTS):
            x_copy(x, p).start()

    e = lax.rem(z - x + planes, SIDE)
    lower = jnp.where(e == 0, SIDE, e)
    upper = SIDE - e

    def across(o):
        return jnp.where(o == 2, 3, jnp.where(o == 3, 2, o))

    def ring(i, carry):
        ib = i - lower
        ia = i - upper
        db = lower + SIDE * (ib // SIDE)
        da = upper + SIDE * (ia // SIDE)
        kb = around(z - db, planes) // SIDE
        ka = around(z + da, planes) // SIDE
        xb = lax.rem(ib + SIDE, SIDE)
        xa = lax.rem(ia + SIDE, SIDE)
        for p in range(PARTS):
            @pl.when(origin & (i < SIDE))
            def _():
                xs = lax.rem(x + across(i), SIDE)
                slot = kq * SIDE + xs

                @pl.when(i > 0)
                def _():
                    x_copy(xs, p).wait_recv()
                up_move(slot, p).start()
                down_move(slot, p).start()
                hand_over(kq, xs, p)

            @pl.when((ib >= 0) & (ib < 2 * SIDE) & ((db < far) | (p < EARLY)))
            def _():
                slot = kb * SIDE + lax.rem(x + across(xb), SIDE)
                up_move(slot, p).wait_recv()

                @pl.when(goes_up(db, p))
                def _():
                    up_move(slot, p).start()
                hand_over(kb, lax.rem(x + across(xb), SIDE), p)

            @pl.when((ia >= 0) & (ia < 2 * SIDE) & ((da < far) | (p >= EARLY)))
            def _():
                slot = ka * SIDE + lax.rem(x + across(xa), SIDE)
                down_move(slot, p).wait_recv()

                @pl.when(goes_down(da, p))
                def _():
                    down_move(slot, p).start()
                hand_over(ka, lax.rem(x + across(xa), SIDE), p)
        return carry

    lax.fori_loop(0, 3 * SIDE, ring, 0)

    def pass_on(xs, carry):
        for o in range(1, SIDE):
            place = around(y + o, SIDE) * SIDE + xs
            whole = fin.at[c, place]
            pltpu.make_async_copy(whole, whole, y_r.at[place]).wait()
            remote(whole, whole, p_s, p_r, here).start()
        return carry

    lax.fori_loop(0, SIDE, pass_on, 0)

    pltpu.make_async_copy(trans, trans, p_r).wait()
    pltpu.make_async_copy(trans, trans, p_s).wait()
    kept = trans.at[pl.ds(0, spots - SIDE)]
    pltpu.make_async_copy(kept, kept, y_s).wait()

    def swept(sem, short, cuts):
        whole = trans.at[pl.ds(0, 2 * SIDE)]
        less = trans.at[pl.ds(0, SIDE * (PARTS + cuts) // 2), pl.ds(0, 2 * cut)]

        @pl.when(short)
        def _():
            pltpu.make_async_copy(less, less, sem).wait()

        @pl.when(~short)
        def _():
            pltpu.make_async_copy(whole, whole, sem).wait()

    swept(up_s, e == SIDE - 1, EARLY)
    swept(down_s, e == 1, PARTS - EARLY)

    @pl.when(~origin)
    def _():
        pltpu.make_async_copy(own, own, x_s).wait()

    pltpu.make_async_copy(tokens.at[1], tokens.at[1], tok_s).wait()
    arrived(z_s, planes - 1 - 2 * NEAR, rcut + pcut, lcut)
    arrived(z_s, 2 * NEAR, rcut + pcut, lcut * (SIDE - 1))
    arrived(a_s, planes - 1 - 2 * NEAR, rcut, lcut * (SIDE - 1))
    arrived(b_s, planes - 1, rcut * (SIDE - 1), lat)
    arrived(b_s, planes - 1, pcut, rows * (SIDE - 1))


def read_kernel(x_ref, up_ref, q_ref, plain_ref, value_ref, rot_ref, read_ref):
    part = pl.program_id(0)
    spots, block, lat = x_ref.shape[1:]
    length, kw = plain_ref.shape[1:]
    rope = rot_ref.shape[1]
    span = length // spots
    fold = block - span
    wide = x_ref[part, :, span:]
    for g in range(rope // fold):
        for n in range(spots):
            rot_ref[0, g * fold:(g + 1) * fold, n * span:(n + 1) * span] = wide[n, :, g * span:(g + 1) * span]
    both = jnp.dot(x_ref[part, :, :span].reshape(length, lat), up_ref[...], preferred_element_type=F32).astype(BF16)
    keys = both[:, :kw]
    values = both[:, kw:]
    plain_ref[0] = keys
    value_ref[0] = values
    chosen = jnp.where(part == 0, q_ref[:1].astype(F32), q_ref[1:].astype(F32)).astype(BF16)
    contract = (((1,), (1,)), ((), ()))
    scores = lax.dot_general(chosen[:, :kw], keys, contract, preferred_element_type=F32)
    scores = scores + jnp.dot(chosen[:, kw:], rot_ref[0], preferred_element_type=F32)
    scores = scores * (1.0 / (kw + rope) ** 0.5)
    weights = jnp.exp(scores - jnp.max(scores, axis=-1, keepdims=True))
    total = jnp.sum(weights, axis=-1, keepdims=True)
    mixed = jnp.dot(weights.astype(BF16), values, preferred_element_type=F32) / total
    row = lax.broadcasted_iota(jnp.int32, read_ref.shape, 0)
    kept = jnp.where(row == part, mixed, read_ref[...].astype(F32))
    read_ref[...] = jnp.where((part > 0) | (row == 0), kept, 0.0).astype(BF16)


def body(planes, spots, tokens, latent_down, rope_weight, norm_scale, key_up, value_up, query):
    span = tokens.shape[1]
    rows, lat = latent_down.shape
    rope = rope_weight.shape[1]
    heads, kw = key_up.shape[1:]
    vw = value_up.shape[2]
    assert heads == 1
    length = spots * span
    block = span + rope * span // lat
    cosine, sine = turn_tables(np.arange(length + 1), rope)
    vmem = pl.BlockSpec(memory_space=pltpu.VMEM)
    hbm = pl.BlockSpec(memory_space=pl.ANY)
    dma = pltpu.SemaphoreType.DMA
    one = pltpu.SemaphoreType.DMA
    x_all, up, asked = pl.pallas_call(
        functools.partial(move_kernel, planes, spots),
        out_shape=(pltpu.VMEM((CORES, spots, block, lat), BF16),
                   pltpu.VMEM((lat, kw + vw), BF16),
                   pltpu.VMEM((CORES, kw + rope), BF16)),
        in_specs=[hbm] * 11,
        out_specs=(vmem, vmem, vmem),
        scratch_shapes=[
            pltpu.VMEM((CORES, planes, span, rows), BF16),
            pltpu.VMEM((planes, rows, lat), BF16),
            pltpu.VMEM((planes, rope, rows), BF16),
            pltpu.VMEM((CORES * span, lat), F32),
            pltpu.VMEM((rope, CORES * span), F32),
            pltpu.VMEM((span, lat), F32),
            pltpu.VMEM((rope, span), F32),
            pltpu.VMEM((block, lat), BF16),
            pltpu.VMEM((spots, block, lat), BF16),
            pltpu.VMEM((rope, span), F32),
            pltpu.VMEM((rope, span), F32),
            pltpu.VMEM((1, lat), F32),
            pltpu.VMEM((CORES, kw + rope), BF16),
            pltpu.VMEM((1, rope), F32),
            pltpu.VMEM((1, rope), F32),
            one, one, one, dma((10,)),
            one, dma((planes,)), one, dma((planes,)),
            one, dma((planes,)),
            dma((2,)), dma((2,)),
            one, dma((PARTS, SIDE)), one, one, dma((PARTS, spots)),
            one, dma((spots,)), one, one,
        ],
        compiler_params=pltpu.CompilerParams(collective_id=0, has_side_effects=True, vmem_limit_bytes=GRANT),
    )(tokens, latent_down, rope_weight.T, norm_scale.reshape(1, lat),
      jnp.asarray(np.ascontiguousarray(cosine[:length].T)), jnp.asarray(np.ascontiguousarray(sine[:length].T)),
      key_up.reshape(lat, kw), value_up.reshape(lat, vw), query.reshape(CORES, kw + rope),
      jnp.asarray(cosine[length:]), jnp.asarray(sine[length:]))

    def whole(shape):
        return pl.BlockSpec(shape, lambda i: (0,) * len(shape))

    def per(shape):
        return pl.BlockSpec((1,) + shape, lambda i: (i,) + (0,) * len(shape))

    plain, value, rot, read = pl.pallas_call(
        read_kernel,
        grid=(CORES,),
        out_shape=(jax.ShapeDtypeStruct((CORES, length, kw), BF16),
                   jax.ShapeDtypeStruct((CORES, length, vw), BF16),
                   jax.ShapeDtypeStruct((CORES, rope, length), BF16),
                   jax.ShapeDtypeStruct((CORES, vw), BF16)),
        in_specs=[vmem, vmem, vmem],
        out_specs=(per((length, kw)), per((length, vw)), per((rope, length)), whole((CORES, vw))),
        compiler_params=pltpu.CompilerParams(vmem_limit_bytes=READ_GRANT),
    )(x_all, up, asked)
    return (plain.reshape(CORES, length, heads, kw), value.reshape(CORES, length, heads, vw), jnp.swapaxes(rot, 1, 2),
            read.reshape(CORES, heads, vw))


def solution(mesh):
    planes = mesh.shape["tp"] // CORES
    spots = mesh.shape["sp"]
    assert planes == spots == SIDE * SIDE
    in_specs = (
        P("tp", "sp", None),
        P("tp", None),
        P("tp", None),
        P(),
        P(None, "tp", None),
        P(None, "tp", None),
        P("sp", "tp", None),
    )
    out_specs = (
        P("sp", None, "tp", None),
        P("sp", None, "tp", None),
        P("sp", None, None),
        P("sp", "tp", None),
    )
    return jax.shard_map(functools.partial(body, planes, spots), mesh=mesh, in_specs=in_specs,
                         out_specs=out_specs, check_vma=False)
```
